32 devices in a mesh: grp: 2 (over y), ep: 4 (over z), tp: 4 (over x, core).
Axes of the slice: x: 2, y: 2, z: 4, core: 2. Of those that a mesh axis runs over, the one named last changes fastest.
Arguments:
- hidden_in: bfloat16 [4096, 2048], P(('grp', 'ep', 'tp')), parts along dimension 0, may hold values from -6 to 6
- expert_ids: int32 [4096, 2], P(('grp', 'ep', 'tp')), parts along dimension 0, may hold values from 0 to 15, all different within a row; in each aligned block of 128 rows (0 to 127, 128 to 255, ...) at most 32 rows name the same one
- route_weights: float32 [4096, 2], P(('grp', 'ep', 'tp')), parts along dimension 0, may hold values from 0.1 to 1
- norm_gain: float32 [2048], replicated, may hold values from 0.1 to 1.9
- gate_proj: bfloat16 [16, 2048, 512], P(('ep', 'tp')), may hold values from -0.125 to 0.125
- up_proj: bfloat16 [16, 2048, 512], P(('ep', 'tp')), may hold values from -0.125 to 0.125
- down_proj: bfloat16 [16, 512, 2048], P(('ep', 'tp')), may hold values from -0.25 to 0.25
Outputs:
- mixed_out: bfloat16 [4096, 2048], P(('grp', 'ep', 'tp')), parts along dimension 0
The draws below stay inside these ranges and needn't reach their ends.
There are 2 independent parts, one for each index of `grp`. The reference program is written for one: setup_inputs(seed, part) draws one part's arguments, and reference() takes and returns one part's arrays. A program takes and returns all parts, laid end to end along the dimension named above; an argument that names none is the same for every part. Nothing has to cross between parts.
Inputs may be any that keep to these rules, and one draw needn't show every extreme that they name: `expert_ids`: each token names 2 different experts; among the 128 tokens of one device (aligned blocks of rows) no expert is named more than 32 times, and in every draw some expert is named exactly 32 times by some device's tokens.
All inputs are finite; a program needn't handle non-finite values.
Results may differ from the reference program's by a relative error of at most 0.0071.
Values may be sent and summed in bfloat16 or wider, within the bound.
No kernel may reach another device: no remote copies, remote signals or barrier semaphores. Data moves between devices by JAX's collectives and lax.ppermute only.
A program may use at most 64 MiB of HBM per device.

```python
import math
import jax
import jax.numpy as jnp
import numpy as np
from jax import lax

D = 2048
FE = 512
TOP_K = 2
TOK_DEV = 128
EXPERTS = 16
TOKENS = 2048
CAP = 32
N_EP = 4
N_TP = 4


def block_levels(stream_key, shape, cuts, least, high):
    gain, own = 1.0, jax.random.fold_in(stream_key, 6)
    for dim, blocks in cuts:
        steps = jnp.exp(jax.random.uniform(jax.random.fold_in(own, dim), (blocks,), jnp.float32, least / len(cuts), high / len(cuts)))
        gain = gain * jnp.repeat(steps, shape[dim] // blocks).reshape([-1 if axis == dim else 1 for axis in range(len(shape))])
    return gain


def shared_out(key, own, number, rows, amount, top, reach, lean):
    ranking = jax.random.permutation(key, amount)
    packed, ordinary = portions_of(amount, rows * top, reach, lean, True), portions_of(amount, rows * top, reach, lean, False)
    places = jnp.arange(amount)

    def named(lengths, offset_by):
        used = int((lengths > 0).sum())
        fixed = max(1, used // 4)
        passed = fixed + (places - fixed + offset_by * (used - fixed)) % max(1, amount - fixed)
        return jnp.zeros((amount,), jnp.int32).at[ranking[jnp.where(places < fixed, places, passed)]].set(jnp.asarray(lengths, jnp.int32))

    lengths = jnp.where(number % 4 == 0, named(packed, number // 4), named(ordinary, number - number // 4 - 1))
    mixed = jax.random.permutation(jax.random.fold_in(own, 3), amount)
    donor, taker = mixed[0:amount // 2 * 2:2], mixed[1:amount // 2 * 2:2]
    room = jnp.minimum(lengths[donor] - 1, reach - lengths[taker]) // 2
    room = jnp.where((donor == ranking[0]) | (taker == ranking[0]) | (lengths[taker] == 0), 0, jnp.maximum(room, 0))
    passed = jax.random.randint(jax.random.fold_in(own, 4), (amount // 2,), 0, 1 << 20) % (room + 1)
    lengths = lengths.at[donor].add(-passed).at[taker].add(passed)
    labels = jnp.searchsorted(jnp.cumsum(lengths), jnp.arange(rows * top), side="right").astype(jnp.int32)
    listing = labels.reshape(top, rows).T
    listing = listing[jax.random.permutation(jax.random.fold_in(own, 1), rows)]
    offset_by = jax.random.randint(jax.random.fold_in(own, 2), (rows, 1), 0, top)
    return jnp.take_along_axis(listing, (jnp.arange(top)[None, :] + offset_by) % top, axis=1)


def portions_of(amount, total, most, lean, full):
    weights = [(1 << 20) // math.isqrt(rank ** lean) + 1 for rank in range(1, amount + 1)]
    largest = most if full else min(most, max(-(-total // amount), total * weights[0] // sum(weights)))
    least = 1 if total - largest >= amount - 1 else 0
    given, surplus = [largest] + [least] * (amount - 1), total - largest - least * (amount - 1)
    while surplus > 0:
        free = [i for i in range(1, amount) if given[i] < largest] or [i for i in range(1, amount) if given[i] < most]
        mass, remaining = sum([weights[i] for i in free]), surplus
        for i in free:
            addition = min(most - given[i], max(1, remaining * weights[i] // mass), surplus)
            given[i] = given[i] + addition
            surplus = surplus - addition
    return np.array(given)


def gaussian(stream_key, extent, deviation, most, split=(), held_as=jnp.bfloat16):
    result = jax.random.normal(stream_key, extent, jnp.float32) * deviation
    if len(split) > 0:
        result = block_levels(stream_key, extent, split, -0.22, 0.18) * result
    return jnp.clip(result, min=-most, max=most).astype(held_as)


def setup_inputs(seed: int = 0, part: int = 0) -> dict:
    splits = jax.random.split(jax.random.key(seed), 8)
    own_keys = jax.random.split(jax.random.fold_in(splits[7], part), 8)
    hidden_in = gaussian(own_keys[0], (TOKENS, D), 1.0, 6.0, ((0, 16),))
    expert_ids_keys = jax.random.split(jax.random.fold_in(own_keys[1], 1), TOKENS // TOK_DEV)
    expert_ids_turns = jax.random.permutation(jax.random.fold_in(own_keys[1], 3), TOKENS // TOK_DEV)
    expert_ids = jax.vmap(lambda own, number: shared_out(jax.random.fold_in(own_keys[1], 2), own, number, TOK_DEV, EXPERTS, TOP_K, CAP, 2))(expert_ids_keys, expert_ids_turns).reshape((TOKENS, TOP_K))
    route_weights = jnp.clip(jnp.exp(math.log(1.0) - 2.3025851 * jax.random.uniform(own_keys[2], (TOKENS, TOP_K), jnp.float32) ** block_levels(own_keys[2], (TOKENS, TOP_K), ((0, 16),), -0.2, 0.2)), 0.1, 1.0)
    norm_gain = jnp.clip(1.0 + 0.18 * jax.random.normal(splits[3], (D,), jnp.float32), 0.1, 1.9)
    gate_proj = gaussian(splits[4], (EXPERTS, D, FE), D ** -0.5, 0.125, ((0, 16),))
    up_proj = gaussian(splits[5], (EXPERTS, D, FE), D ** -0.5, 0.125, ((0, 16),))
    down_proj = gaussian(splits[6], (EXPERTS, FE, D), FE ** -0.5, 0.25, ((0, 16),))
    return dict(hidden_in=hidden_in, expert_ids=expert_ids, route_weights=route_weights, norm_gain=norm_gain, gate_proj=gate_proj, up_proj=up_proj, down_proj=down_proj)


def reference(hidden_in, expert_ids, route_weights, norm_gain, gate_proj, up_proj, down_proj):
    device_count = N_EP * N_TP
    as_float = hidden_in.astype(jnp.float32)
    scaled = as_float * lax.rsqrt(lax.optimization_barrier(jnp.mean(as_float * as_float, axis=-1, keepdims=True)) + 1e-06)
    normed = (scaled * norm_gain).astype(jnp.bfloat16)
    flat_ids = expert_ids.reshape(device_count, TOK_DEV * TOP_K).astype(jnp.int32)
    onehot = (flat_ids[:, :, None] == jnp.arange(EXPERTS, dtype=jnp.int32)[None, None, :]).astype(jnp.int32)
    slot_index = lax.optimization_barrier(jnp.sum((jnp.cumsum(onehot, axis=1) - onehot) * onehot, axis=2)).astype(jnp.int32)
    source = jnp.arange(device_count, dtype=jnp.int32)[:, None]
    target = (flat_ids * (device_count * CAP) + source * CAP + slot_index).reshape(-1).astype(jnp.int32)
    routed = jnp.repeat(normed, TOP_K, axis=0)
    expert_rows = jnp.zeros((EXPERTS * device_count * CAP, D), jnp.bfloat16).at[target].set(routed)
    expert_rows = expert_rows.reshape(EXPERTS, device_count * CAP, D)

    def run_expert(pieces):
        block_in, weight_gate, weight_up, weight_down = pieces
        block_float = block_in.astype(jnp.float32)
        gate_act = jnp.dot(block_float, weight_gate.astype(jnp.float32))
        up_act = jnp.dot(block_float, weight_up.astype(jnp.float32))
        hidden = (jax.nn.silu(gate_act) * up_act).astype(jnp.bfloat16)
        return jnp.dot(hidden.astype(jnp.float32), weight_down.astype(jnp.float32)).astype(jnp.bfloat16)
    expert_out = lax.map(run_expert, (expert_rows, gate_proj, up_proj, down_proj))
    picked = expert_out.reshape(-1, D)[target].astype(jnp.float32).reshape(TOKENS, TOP_K, D)
    return lax.optimization_barrier(jnp.sum(picked * route_weights[:, :, None], axis=1)).astype(jnp.bfloat16)
```

```python
import functools

import jax
import jax.numpy as jnp
from jax import lax
from jax.experimental import pallas as pl
from jax.experimental.pallas import tpu as pltpu
from jax.sharding import PartitionSpec as P


def targets_of(ids_ref, expert_count, capacity):
    choose_count, token_count = ids_ref.shape
    experts = lax.broadcasted_iota(jnp.int32, (expert_count, token_count), 0)
    named = [ids_ref[k : k + 1, :] == experts for k in range(choose_count)]
    either = functools.reduce(jnp.logical_or, named).astype(jnp.float32).astype(jnp.bfloat16)
    earlier = lax.broadcasted_iota(jnp.int32, (token_count, token_count), 0) < (
        lax.broadcasted_iota(jnp.int32, (token_count, token_count), 1)
    )
    earlier = earlier.astype(jnp.float32).astype(jnp.bfloat16)
    before = jnp.dot(either, earlier, preferred_element_type=jnp.float32)
    targets = []
    for k in range(choose_count):
        slot = jnp.sum(jnp.where(named[k], before, 0.0), axis=0, keepdims=True)
        targets.append(ids_ref[k : k + 1, :] * capacity + slot.astype(jnp.int32))
    return targets


def as_ones(mask):
    return mask.astype(jnp.float32).astype(jnp.bfloat16)


def dispatch_kernel(expert_count, capacity, hidden_ref, ids_ref, gain_ref, buffer_ref):
    as_float = hidden_ref[...].astype(jnp.float32)
    mean = jnp.mean(as_float * as_float, axis=-1, keepdims=True)
    normed = (as_float * lax.rsqrt(mean + 1e-06) * gain_ref[...]).astype(jnp.bfloat16)
    targets = targets_of(ids_ref, expert_count, capacity)
    rows = lax.broadcasted_iota(jnp.int32, (expert_count * capacity, ids_ref.shape[1]), 0)
    chosen = as_ones(functools.reduce(jnp.logical_or, [rows == target for target in targets]))
    buffer_ref[...] = jnp.dot(chosen, normed, preferred_element_type=jnp.float32).astype(jnp.bfloat16)


def expert_kernel(rows_ref, gate_ref, up_ref, down_ref, out_ref):
    block = rows_ref[...]
    gate_act = jnp.dot(block, gate_ref[0], preferred_element_type=jnp.float32)
    up_act = jnp.dot(block, up_ref[0], preferred_element_type=jnp.float32)
    hidden = (gate_act / (1.0 + jnp.exp(-gate_act)) * up_act).astype(jnp.bfloat16)
    out_ref[...] = jnp.dot(hidden, down_ref[0], preferred_element_type=jnp.float32).astype(jnp.bfloat16)


def combine_kernel(expert_count, capacity, rows_ref, ids_ref, weights_ref, out_ref):
    token_count = ids_ref.shape[1]
    targets = targets_of(ids_ref, expert_count, capacity)
    rows = lax.broadcasted_iota(jnp.int32, (expert_count * capacity, token_count), 0)
    total = None
    for k, target in enumerate(targets):
        picked = lax.dot_general(
            as_ones(rows == target), rows_ref[...], (((0,), (0,)), ((), ())), preferred_element_type=jnp.float32
        )
        weight = jnp.broadcast_to(weights_ref[k : k + 1, :], (8, token_count)).T[:, 0:1]
        total = picked * weight if total is None else total + picked * weight
    out_ref[...] = total.astype(jnp.bfloat16)


def whole(*arrays):
    return [pl.BlockSpec(a.shape, lambda *_, n=len(a.shape): (0,) * n) for a in arrays]


def body(hidden_in, expert_ids, route_weights, norm_gain, gate_proj, up_proj, down_proj):
    token_count, model_width = hidden_in.shape
    choose_count = expert_ids.shape[1]
    expert_count = lax.axis_size("ep") * lax.axis_size("tp")
    capacity = max(2, 2 * choose_count * token_count // expert_count)
    slots = expert_count * capacity
    ids, weights, gain = expert_ids.T, route_weights.T, norm_gain[None, :]
    buffer = pl.pallas_call(
        functools.partial(dispatch_kernel, expert_count, capacity),
        out_shape=jax.ShapeDtypeStruct((slots, model_width), jnp.bfloat16),
        name="dispatch",
    )(hidden_in, ids, gain)
    buffer = buffer.reshape(expert_count, capacity, model_width)
    arrived = lax.all_to_all(buffer, ("ep", "tp"), split_axis=0, concat_axis=0, tiled=True)
    arrived = arrived.reshape(slots, model_width)
    tile = slots // 2 if slots % 32 == 0 else slots
    result = pl.pallas_call(
        expert_kernel,
        grid=(slots // tile,),
        in_specs=[pl.BlockSpec((tile, model_width), lambda i: (i, 0)), *whole(gate_proj, up_proj, down_proj)],
        out_specs=pl.BlockSpec((tile, model_width), lambda i: (i, 0)),
        out_shape=jax.ShapeDtypeStruct((slots, model_width), jnp.bfloat16),
        name="experts",
    )(arrived, gate_proj, up_proj, down_proj)
    results = result.reshape(expert_count, capacity, model_width)
    returned = lax.all_to_all(results, ("ep", "tp"), split_axis=0, concat_axis=0, tiled=True)
    return pl.pallas_call(
        functools.partial(combine_kernel, expert_count, capacity),
        out_shape=jax.ShapeDtypeStruct((token_count, model_width), jnp.bfloat16),
        name="combine",
    )(returned.reshape(slots, model_width), ids, weights)


def solution(mesh):
    return jax.shard_map(
        body,
        mesh=mesh,
        in_specs=(
            P(("grp", "ep", "tp"), None),
            P(("grp", "ep", "tp"), None),
            P(("grp", "ep", "tp"), None),
            P(),
            P(("ep", "tp"), None, None),
            P(("ep", "tp"), None, None),
            P(("ep", "tp"), None, None),
        ),
        out_specs=P(("grp", "ep", "tp"), None),
        check_vma=False,
    )
```

```python
import functools

import jax
import jax.numpy as jnp
from jax import lax
from jax.experimental import pallas as pl
from jax.experimental.pallas import tpu as pltpu
from jax.sharding import Mesh, PartitionSpec as P


SMEM = pl.BlockSpec(memory_space=pltpu.SMEM)
VMEM = pl.BlockSpec(memory_space=pltpu.VMEM)
HBM = pl.BlockSpec(memory_space=pl.ANY)
LIMIT = pltpu.CompilerParams(vmem_limit_bytes=32 * 1024 * 1024)


def as_ones(mask):
    return mask.astype(jnp.float32).astype(jnp.bfloat16)


def any_of(masks):
    return functools.reduce(jnp.logical_or, masks)


def slots_of(ids, expert_count):
    choose_count, token_count = ids.shape
    experts = lax.broadcasted_iota(jnp.int32, (expert_count, token_count), 0)
    named = [ids[k : k + 1, :] == experts for k in range(choose_count)]
    earlier = as_ones(
        lax.broadcasted_iota(jnp.int32, (token_count, token_count), 0)
        < lax.broadcasted_iota(jnp.int32, (token_count, token_count), 1)
    )
    before = jnp.dot(as_ones(any_of(named)), earlier, preferred_element_type=jnp.float32)
    return [jnp.sum(jnp.where(mask, before, 0.0), axis=0, keepdims=True).astype(jnp.int32) for mask in named]


def marks_of(ids, slots, first, turn, count, capacity):
    rows = lax.broadcasted_iota(jnp.int32, (count * capacity, ids.shape[1]), 0)
    targets = []
    for k, slot in enumerate(slots):
        expert = ids[k : k + 1, :] - first
        inside = (expert >= 0) & (expert < count)
        targets.append(jnp.where(inside, (expert ^ turn) * capacity + slot, -1))
    return [rows == target for target in targets]


def column_of(row):
    return jnp.broadcast_to(row, (8, row.shape[1])).T[:, 0:1]


def pick(marks, weights, rows):
    total = None
    for k, mark in enumerate(marks):
        picked = lax.dot_general(mark, rows, (((0,), (0,)), ((), ())), preferred_element_type=jnp.float32)
        picked = picked * column_of(weights[k : k + 1, :])
        total = picked if total is None else total + picked
    return total


def together(refs):
    return jnp.concatenate([ref[...] for ref in refs], axis=0) if len(refs) > 1 else refs[0][...]


def apart(value, refs):
    size = value.shape[0] // len(refs)
    for i, ref in enumerate(refs):
        ref[...] = value[i * size : (i + 1) * size].astype(ref.dtype)


def norm_kernel(hidden_ref, gain_ref, ids_ref, weights_ref, out_ref):
    as_float = hidden_ref[...].astype(jnp.float32)
    scale = lax.rsqrt(jnp.mean(as_float * as_float, axis=-1, keepdims=True) + 1e-06)
    width = hidden_ref.shape[1]
    out_ref[:, :width] = (as_float * scale * gain_ref[...]).astype(jnp.bfloat16)
    facts, left = [ids_ref[...].astype(jnp.float32)], weights_ref[...]
    for _ in range(3):
        term = left.astype(jnp.bfloat16).astype(jnp.float32)
        facts.append(term)
        left = left - term
    facts.append(jnp.zeros((LANES - 4 * ids_ref.shape[0], ids_ref.shape[1]), jnp.float32))
    out_ref[:, width:] = jnp.concatenate(facts, axis=0).T.astype(jnp.bfloat16)


def facts_of(block_ref, choose_count):
    facts = block_ref[:, block_ref.shape[1] - LANES :].astype(jnp.float32).T
    terms = [facts[(1 + i) * choose_count : (2 + i) * choose_count, :] for i in range(3)]
    return facts[:choose_count, :].astype(jnp.int32), terms[0] + terms[1] + terms[2]


def pack_kernel(layout, keep, place_ref, block_ref, *refs):
    choose_count, expert_count, count, capacity = layout
    ids, weights = facts_of(block_ref, choose_count)
    marks = marks_of(ids, slots_of(ids, expert_count), place_ref[0], place_ref[1], count, capacity)
    if keep:
        for k, mark in enumerate(marks):
            refs[0][k] = as_ones(mark)
        refs[1][...] = weights
    rows = block_ref[:, : block_ref.shape[1] - LANES]
    apart(jnp.dot(as_ones(any_of(marks)), rows, preferred_element_type=jnp.float32), refs[2 * keep :])


def mark_kernel(layout, place_ref, ids_ref, out_ref):
    _, expert_count, count, capacity = layout
    ids = ids_ref[...]
    marks = marks_of(ids, slots_of(ids, expert_count), place_ref[0], place_ref[1], count, capacity)
    for k, mark in enumerate(marks):
        out_ref[k] = as_ones(mark)


def expert_kernel(count, *refs):
    weight_refs, in_refs, out_refs = refs[:3], refs[3 : 3 + count], refs[3 + count : 3 + 2 * count]
    *held, sems = refs[3 + 2 * count :]
    loads = [pltpu.make_async_copy(weight_refs[i].at[0], held[i], sems.at[i]) for i in range(3)]
    for load in loads:
        load.start()
    rows = together(in_refs)
    loads[0].wait()
    gate_act = jnp.dot(rows, held[0][...], preferred_element_type=jnp.float32)
    loads[1].wait()
    up_act = jnp.dot(rows, held[1][...], preferred_element_type=jnp.float32)
    hidden = (gate_act / (1.0 + jnp.exp(-gate_act)) * up_act).astype(jnp.bfloat16)
    loads[2].wait()
    apart(jnp.dot(hidden, held[2][...], preferred_element_type=jnp.float32), out_refs)


def partial_kernel(weights_ref, marks_ref, *refs):
    out = pick([marks_ref[k] for k in range(marks_ref.shape[0])], weights_ref[...], together(refs[:-1]))
    refs[-1][...] = out.astype(jnp.bfloat16)


def final_kernel(weights_ref, marks_ref, partial_ref, *refs):
    near = pick([marks_ref[k] for k in range(marks_ref.shape[0])], weights_ref[...], together(refs[:-1]))
    refs[-1][...] = (near + partial_ref[...].astype(jnp.float32)).astype(jnp.bfloat16)


LANES = 128


def body(hidden_in, expert_ids, route_weights, norm_gain, gate_proj, up_proj, down_proj):
    token_count, model_width = hidden_in.shape
    choose_count = expert_ids.shape[1]
    half_count = lax.axis_size("el") * lax.axis_size("tp")
    expert_count = lax.axis_size("eh") * half_count
    capacity = max(2, 2 * choose_count * token_count // expert_count)
    slots = half_count * capacity
    group = ("el", "tp")
    paired = half_count <= 8 and half_count & (half_count - 1) == 0 and capacity % 16 == 0
    turn = lax.axis_index(group) if paired else jnp.int32(0)
    place = jnp.stack([lax.axis_index("eh") * half_count, turn]).astype(jnp.int32)
    ids, weights, gain = expert_ids.T, route_weights.T, norm_gain[None, :]
    proj = [pltpu.with_memory_space_constraint(w, pltpu.HBM) for w in (gate_proj, up_proj, down_proj)]

    def array(*shape):
        return pltpu.HBM(shape, jnp.bfloat16)

    def call(kernel, scalars, out, *args, limit=LIMIT):
        return pl.pallas_call(
            kernel,
            in_specs=[SMEM] * scalars + [VMEM] * (len(args) - scalars),
            out_specs=[VMEM] * len(out),
            out_shape=out,
            compiler_params=limit,
        )(*args)

    def cross(value):
        return lax.ppermute(value, "eh", [(0, 1), (1, 0)])

    def scatter(parts):
        if not paired:
            blocks = parts[0].reshape(half_count, capacity, model_width)
            blocks = lax.all_to_all(blocks, group, split_axis=0, concat_axis=0, tiled=True)
            return [blocks.reshape(slots, model_width)]
        moved = [parts[0]]
        for j in range(1, len(parts)):
            moved.append(lax.ppermute(parts[j], group, [(i, i ^ j) for i in range(half_count)]))
        return moved

    def experts(rows):
        return pl.pallas_call(
            functools.partial(expert_kernel, len(rows)),
            in_specs=[HBM] * 3 + [VMEM] * len(rows),
            out_specs=[VMEM] * len(rows),
            out_shape=[array(*r.shape) for r in rows],
            scratch_shapes=[
                *[pltpu.VMEM(w.shape[1:], w.dtype) for w in proj],
                pltpu.SemaphoreType.DMA((3,)),
            ],
            compiler_params=LIMIT,
        )(*proj, *rows)

    pieces = half_count if paired else 1
    piece = array(slots // pieces, model_width)
    marks = array(choose_count, slots, token_count)
    layout = (choose_count, expert_count, half_count, capacity)
    (block,) = call(
        norm_kernel, 0, [array(token_count, model_width + LANES)], hidden_in, gain, ids, weights, limit=None
    )
    far_block = cross(block)
    kernel = functools.partial(pack_kernel, layout, False)
    near = scatter(call(kernel, 1, [piece] * pieces, place, block, limit=None))
    (near_marks,) = call(functools.partial(mark_kernel, layout), 1, [marks], place, ids)
    far_marks, far_weights, *far = call(
        functools.partial(pack_kernel, layout, True),
        1,
        [marks, pltpu.HBM((choose_count, token_count), jnp.float32)] + [piece] * pieces,
        place, far_block,
    )
    far = scatter(far)
    near = experts(near)
    far = experts(far)
    far = scatter(far)
    near = scatter(near)
    (partial,) = call(partial_kernel, 0, [array(token_count, model_width)], far_weights, far_marks, *far)
    partial = cross(partial)
    out = jax.ShapeDtypeStruct((token_count, model_width), jnp.bfloat16)
    return call(final_kernel, 0, [out], weights, near_marks, partial, *near)[0]


def solution(mesh):
    sizes = dict(mesh.shape)
    split = Mesh(mesh.devices.reshape(sizes["grp"], 2, sizes["ep"] // 2, sizes["tp"]), ("grp", "eh", "el", "tp"))
    rows, experts = P(("grp", "eh", "el", "tp"), None), P(("eh", "el", "tp"), None, None)

    def step(*args):
        return body(*args)

    step = jax.shard_map(
        step,
        mesh=split,
        in_specs=(rows, rows, rows, P(), experts, experts, experts),
        out_specs=rows,
        check_vma=False,
    )
    return step
```

```python
import functools

import jax
import jax.numpy as jnp
from jax import lax
from jax.experimental import pallas as pl
from jax.experimental.pallas import tpu as pltpu
from jax.sharding import Mesh, PartitionSpec as P


SMEM = pl.BlockSpec(memory_space=pltpu.SMEM)
VMEM = pl.BlockSpec(memory_space=pltpu.VMEM)
HBM = pl.BlockSpec(memory_space=pl.ANY)
LIMIT = pltpu.CompilerParams(vmem_limit_bytes=32 * 1024 * 1024)


def as_ones(mask):
    return mask.astype(jnp.float32).astype(jnp.bfloat16)


def any_of(masks):
    return functools.reduce(jnp.logical_or, masks)


def slots_of(ids, expert_count):
    choose_count, token_count = ids.shape
    experts = lax.broadcasted_iota(jnp.int32, (expert_count, token_count), 0)
    named = [ids[k : k + 1, :] == experts for k in range(choose_count)]
    earlier = as_ones(
        lax.broadcasted_iota(jnp.int32, (token_count, token_count), 0)
        < lax.broadcasted_iota(jnp.int32, (token_count, token_count), 1)
    )
    before = jnp.dot(as_ones(any_of(named)), earlier, preferred_element_type=jnp.float32)
    return [jnp.sum(jnp.where(mask, before, 0.0), axis=0, keepdims=True).astype(jnp.int32) for mask in named]


def marks_of(ids, slots, first, turn, count, capacity):
    rows = lax.broadcasted_iota(jnp.int32, (count * capacity, ids.shape[1]), 0)
    targets = []
    for k, slot in enumerate(slots):
        expert = ids[k : k + 1, :] - first
        inside = (expert >= 0) & (expert < count)
        targets.append(jnp.where(inside, (expert ^ turn) * capacity + slot, -1))
    return [rows == target for target in targets]


def column_of(row):
    return jnp.broadcast_to(row, (8, row.shape[1])).T[:, 0:1]


def pick(marks, weights, rows):
    total = None
    for k, mark in enumerate(marks):
        picked = lax.dot_general(mark, rows, (((0,), (0,)), ((), ())), preferred_element_type=jnp.float32)
        picked = picked * column_of(weights[k : k + 1, :])
        total = picked if total is None else total + picked
    return total


def together(refs):
    return jnp.concatenate([ref[...] for ref in refs], axis=0) if len(refs) > 1 else refs[0][...]


def apart(value, refs):
    size = value.shape[0] // len(refs)
    for i, ref in enumerate(refs):
        ref[...] = value[i * size : (i + 1) * size].astype(ref.dtype)


def normed_of(hidden_ref, gain_ref):
    as_float = hidden_ref[...].astype(jnp.float32)
    scale = lax.rsqrt(jnp.mean(as_float * as_float, axis=-1, keepdims=True) + 1e-06)
    return (as_float * scale * gain_ref[...]).astype(jnp.bfloat16)


def near_kernel(layout, place_ref, hidden_ref, gain_ref, ids_ref, *out_refs):
    expert_count, count, capacity = layout
    ids = ids_ref[...]
    marks = marks_of(ids, slots_of(ids, expert_count), place_ref[0], place_ref[1], count, capacity)
    rows = normed_of(hidden_ref, gain_ref)
    apart(jnp.dot(as_ones(any_of(marks)), rows, preferred_element_type=jnp.float32), out_refs)


def mark_kernel(layout, place_ref, *refs):
    expert_count, count, capacity = layout
    for ids_ref, out_ref in zip(refs[:2], refs[2:]):
        ids = ids_ref[...]
        marks = marks_of(ids, slots_of(ids, expert_count), place_ref[0], place_ref[1], count, capacity)
        for k, mark in enumerate(marks):
            out_ref[k] = as_ones(mark)


def far_kernel(hidden_ref, gain_ref, marks_ref, *out_refs):
    chosen = functools.reduce(jnp.add, [marks_ref[k] for k in range(marks_ref.shape[0])])
    rows = normed_of(hidden_ref, gain_ref)
    apart(jnp.dot(chosen, rows, preferred_element_type=jnp.float32), out_refs)


def expert_kernel(count, *refs):
    weight_refs, in_refs, out_refs = refs[:3], refs[3 : 3 + count], refs[3 + count : 3 + 2 * count]
    *held, sems = refs[3 + 2 * count :]
    loads = [pltpu.make_async_copy(weight_refs[i].at[0], held[i], sems.at[i]) for i in range(3)]
    for load in loads:
        load.start()
    rows = together(in_refs)
    loads[0].wait()
    gate_act = jnp.dot(rows, held[0][...], preferred_element_type=jnp.float32)
    loads[1].wait()
    up_act = jnp.dot(rows, held[1][...], preferred_element_type=jnp.float32)
    hidden = (gate_act / (1.0 + jnp.exp(-gate_act)) * up_act).astype(jnp.bfloat16)
    loads[2].wait()
    apart(jnp.dot(hidden, held[2][...], preferred_element_type=jnp.float32), out_refs)


def partial_kernel(weights_ref, marks_ref, *refs):
    out = pick([marks_ref[k] for k in range(marks_ref.shape[0])], weights_ref[...], together(refs[:-1]))
    refs[-1][...] = out.astype(jnp.bfloat16)


def final_kernel(weights_ref, marks_ref, partial_ref, *refs):
    near = pick([marks_ref[k] for k in range(marks_ref.shape[0])], weights_ref[...], together(refs[:-1]))
    refs[-1][...] = (near + partial_ref[...].astype(jnp.float32)).astype(jnp.bfloat16)


def in_hbm(value):
    return pltpu.with_memory_space_constraint(value, pltpu.HBM)


def body(hidden_in, expert_ids, route_weights, norm_gain, gate_proj, up_proj, down_proj):
    token_count, model_width = hidden_in.shape
    choose_count = expert_ids.shape[1]
    half_count = lax.axis_size("el") * lax.axis_size("tp")
    expert_count = lax.axis_size("eh") * half_count
    capacity = max(2, 2 * choose_count * token_count // expert_count)
    slots = half_count * capacity
    group = ("el", "tp")
    paired = half_count <= 8 and half_count & (half_count - 1) == 0 and capacity % 16 == 0
    turn = lax.axis_index(group) if paired else jnp.int32(0)
    place = jnp.stack([lax.axis_index("eh") * half_count, turn]).astype(jnp.int32)
    ids, weights, gain = expert_ids.T, route_weights.T, norm_gain[None, :]
    proj = [in_hbm(w) for w in (gate_proj, up_proj, down_proj)]

    def array(*shape):
        return pltpu.HBM(shape, jnp.bfloat16)

    def call(kernel, scalars, out, *args, limit=LIMIT):
        return pl.pallas_call(
            kernel,
            in_specs=[SMEM] * scalars + [VMEM] * (len(args) - scalars),
            out_specs=[VMEM] * len(out),
            out_shape=out,
            compiler_params=limit,
        )(*args)

    def cross(value):
        return lax.ppermute(value, "eh", [(0, 1), (1, 0)])

    def scatter(parts):
        if not paired:
            blocks = parts[0].reshape(half_count, capacity, model_width)
            blocks = lax.all_to_all(blocks, group, split_axis=0, concat_axis=0, tiled=True)
            return [blocks.reshape(slots, model_width)]
        moved = [parts[0]]
        for j in range(1, len(parts)):
            moved.append(lax.ppermute(parts[j], group, [(i, i ^ j) for i in range(half_count)]))
        return moved

    def experts(rows):
        return pl.pallas_call(
            functools.partial(expert_kernel, len(rows)),
            in_specs=[HBM] * 3 + [VMEM] * len(rows),
            out_specs=[VMEM] * len(rows),
            out_shape=[array(*r.shape) for r in rows],
            scratch_shapes=[
                *[pltpu.VMEM(w.shape[1:], w.dtype) for w in proj],
                pltpu.SemaphoreType.DMA((3,)),
            ],
            compiler_params=LIMIT,
        )(*proj, *rows)

    pieces = half_count if paired else 1
    piece = array(slots // pieces, model_width)
    marks = array(choose_count, slots, token_count)
    layout = (expert_count, half_count, capacity)
    far_ids, far_weights = cross(expert_ids).T, cross(route_weights).T
    far_hidden = cross(hidden_in)
    kernel = functools.partial(near_kernel, layout)
    near = call(kernel, 1, [piece] * pieces, place, hidden_in, gain, ids, limit=None)
    near = scatter(near)
    kernel = functools.partial(mark_kernel, layout)
    near_marks, far_marks = call(kernel, 1, [marks, marks], place, ids, far_ids)
    far = scatter(call(far_kernel, 0, [piece] * pieces, far_hidden, in_hbm(gain), in_hbm(far_marks)))
    near = experts(near)
    far = experts(far)
    far = scatter(far)
    near = scatter(near)
    (partial,) = call(partial_kernel, 0, [array(token_count, model_width)], far_weights, far_marks, *far)
    partial = cross(partial)
    out = jax.ShapeDtypeStruct((token_count, model_width), jnp.bfloat16)
    return call(final_kernel, 0, [out], weights, near_marks, partial, *near)[0]


def solution(mesh):
    sizes = dict(mesh.shape)
    split = Mesh(mesh.devices.reshape(sizes["grp"], 2, sizes["ep"] // 2, sizes["tp"]), ("grp", "eh", "el", "tp"))
    rows, experts = P(("grp", "eh", "el", "tp"), None), P(("eh", "el", "tp"), None, None)

    def step(*args):
        return body(*args)

    step = jax.shard_map(
        step,
        mesh=split,
        in_specs=(rows, rows, rows, P(), experts, experts, experts),
        out_specs=rows,
        check_vma=False,
    )
    return step
```

```python
import functools

import jax
import jax.numpy as jnp
from jax import lax
from jax.experimental import pallas as pl
from jax.experimental.pallas import tpu as pltpu
from jax.sharding import Mesh, PartitionSpec as P


SMEM = pl.BlockSpec(memory_space=pltpu.SMEM)
VMEM = pl.BlockSpec(memory_space=pltpu.VMEM)
HBM = pl.BlockSpec(memory_space=pl.ANY)
LIMIT = pltpu.CompilerParams(vmem_limit_bytes=32 * 1024 * 1024)


def as_ones(mask):
    return mask.astype(jnp.float32).astype(jnp.bfloat16)


def any_of(masks):
    return functools.reduce(jnp.logical_or, masks)


def slots_of(ids, expert_count):
    choose_count, token_count = ids.shape
    experts = lax.broadcasted_iota(jnp.int32, (expert_count, token_count), 0)
    named = [ids[k : k + 1, :] == experts for k in range(choose_count)]
    earlier = as_ones(
        lax.broadcasted_iota(jnp.int32, (token_count, token_count), 0)
        < lax.broadcasted_iota(jnp.int32, (token_count, token_count), 1)
    )
    before = jnp.dot(as_ones(any_of(named)), earlier, preferred_element_type=jnp.float32)
    return [jnp.sum(jnp.where(mask, before, 0.0), axis=0, keepdims=True).astype(jnp.int32) for mask in named]


def marks_of(ids, slots, first, turn, count, capacity):
    rows = lax.broadcasted_iota(jnp.int32, (count * capacity, ids.shape[1]), 0)
    targets = []
    for k, slot in enumerate(slots):
        expert = ids[k : k + 1, :] - first
        inside = (expert >= 0) & (expert < count)
        targets.append(jnp.where(inside, (expert ^ turn) * capacity + slot, -1))
    return [rows == target for target in targets]


def column_of(row):
    return jnp.broadcast_to(row, (8, row.shape[1])).T[:, 0:1]


def pick(marks, weights, rows):
    total = None
    for k, mark in enumerate(marks):
        picked = lax.dot_general(mark, rows, (((0,), (0,)), ((), ())), preferred_element_type=jnp.float32)
        picked = picked * column_of(weights[k : k + 1, :])
        total = picked if total is None else total + picked
    return total


def together(refs):
    return jnp.concatenate([ref[...] for ref in refs], axis=0) if len(refs) > 1 else refs[0][...]


def apart(value, refs):
    size = value.shape[0] // len(refs)
    for i, ref in enumerate(refs):
        ref[...] = value[i * size : (i + 1) * size].astype(ref.dtype)


def normed_of(hidden_ref, gain_ref):
    as_float = hidden_ref[...].astype(jnp.float32)
    scale = lax.rsqrt(jnp.mean(as_float * as_float, axis=-1, keepdims=True) + 1e-06)
    return (as_float * scale * gain_ref[...]).astype(jnp.bfloat16)


def near_kernel(layout, place_ref, hidden_ref, gain_ref, ids_ref, *out_refs):
    expert_count, count, capacity = layout
    ids = ids_ref[...]
    marks = marks_of(ids, slots_of(ids, expert_count), place_ref[0], place_ref[1], count, capacity)
    rows = normed_of(hidden_ref, gain_ref)
    apart(jnp.dot(as_ones(any_of(marks)), rows, preferred_element_type=jnp.float32), out_refs)


def mark_kernel(layout, place_ref, gain_ref, near_ids_ref, far_ids_ref, near_ref, far_ref, chosen_ref, held_ref):
    expert_count, count, capacity = layout
    for ids_ref, out_ref in ((near_ids_ref, near_ref), (far_ids_ref, far_ref)):
        ids = ids_ref[...]
        marks = marks_of(ids, slots_of(ids, expert_count), place_ref[0], place_ref[1], count, capacity)
        for k, mark in enumerate(marks):
            out_ref[k] = as_ones(mark)
    chosen_ref[...] = as_ones(any_of(marks))
    held_ref[...] = gain_ref[...]


def far_kernel(hidden_ref, gain_ref, chosen_ref, *out_refs):
    rows = normed_of(hidden_ref, gain_ref)
    apart(jnp.dot(chosen_ref[...], rows, preferred_element_type=jnp.float32), out_refs)


def expert_kernel(count, *refs):
    weight_refs, in_refs, out_refs = refs[:3], refs[3 : 3 + count], refs[3 + count : 3 + 2 * count]
    *held, sems = refs[3 + 2 * count :]
    loads = [pltpu.make_async_copy(weight_refs[i].at[0], held[i], sems.at[i]) for i in range(3)]
    for load in loads:
        load.start()
    rows = together(in_refs)
    loads[0].wait()
    gate_act = jnp.dot(rows, held[0][...], preferred_element_type=jnp.float32)
    loads[1].wait()
    up_act = jnp.dot(rows, held[1][...], preferred_element_type=jnp.float32)
    hidden = (gate_act / (1.0 + jnp.exp(-gate_act)) * up_act).astype(jnp.bfloat16)
    loads[2].wait()
    apart(jnp.dot(hidden, held[2][...], preferred_element_type=jnp.float32), out_refs)


def partial_kernel(weights_ref, marks_ref, *refs):
    out = pick([marks_ref[k] for k in range(marks_ref.shape[0])], weights_ref[...], together(refs[:-1]))
    refs[-1][...] = out.astype(jnp.bfloat16)


def final_kernel(weights_ref, marks_ref, partial_ref, *refs):
    near = pick([marks_ref[k] for k in range(marks_ref.shape[0])], weights_ref[...], together(refs[:-1]))
    refs[-1][...] = (near + partial_ref[...].astype(jnp.float32)).astype(jnp.bfloat16)


def in_hbm(value):
    return pltpu.with_memory_space_constraint(value, pltpu.HBM)


def body(hidden_in, expert_ids, route_weights, norm_gain, gate_proj, up_proj, down_proj):
    token_count, model_width = hidden_in.shape
    choose_count = expert_ids.shape[1]
    half_count = lax.axis_size("el") * lax.axis_size("tp")
    expert_count = lax.axis_size("eh") * half_count
    capacity = max(2, 2 * choose_count * token_count // expert_count)
    slots = half_count * capacity
    group = ("el", "tp")
    paired = half_count <= 8 and half_count & (half_count - 1) == 0 and capacity % 16 == 0
    turn = lax.axis_index(group) if paired else jnp.int32(0)
    place = jnp.stack([lax.axis_index("eh") * half_count, turn]).astype(jnp.int32)
    ids, weights, gain = expert_ids.T, route_weights.T, norm_gain[None, :]
    proj = [in_hbm(w) for w in (gate_proj, up_proj, down_proj)]

    def array(*shape):
        return pltpu.HBM(shape, jnp.bfloat16)

    def call(kernel, scalars, out, *args, limit=LIMIT):
        return pl.pallas_call(
            kernel,
            in_specs=[SMEM] * scalars + [VMEM] * (len(args) - scalars),
            out_specs=[VMEM] * len(out),
            out_shape=out,
            compiler_params=limit,
        )(*args)

    def cross(value):
        return lax.ppermute(value, "eh", [(0, 1), (1, 0)])

    def scatter(parts):
        if not paired:
            blocks = parts[0].reshape(half_count, capacity, model_width)
            blocks = lax.all_to_all(blocks, group, split_axis=0, concat_axis=0, tiled=True)
            return [blocks.reshape(slots, model_width)]
        moved = [parts[0]]
        for j in range(1, len(parts)):
            moved.append(lax.ppermute(parts[j], group, [(i, i ^ j) for i in range(half_count)]))
        return moved

    def experts(name, rows):
        own = [pltpu.VMEM(rows[0].shape, jnp.bfloat16)] if paired and name == "far_experts" else []
        return pl.pallas_call(
            functools.partial(expert_kernel, len(rows)),
            in_specs=[HBM] * 3 + [VMEM] * len(rows),
            out_specs=[VMEM] * len(rows),
            out_shape=[*own, *[array(*r.shape) for r in rows[len(own) :]]],
            scratch_shapes=[
                *[pltpu.VMEM(w.shape[1:], w.dtype) for w in proj],
                pltpu.SemaphoreType.DMA((3,)),
            ],
            compiler_params=LIMIT,
        )(*proj, *rows)

    pieces = half_count if paired else 1
    piece = array(slots // pieces, model_width)
    marks = array(choose_count, slots, token_count)
    layout = (expert_count, half_count, capacity)
    far_ids, far_weights = cross(expert_ids).T, cross(route_weights).T
    far_hidden = cross(hidden_in)
    kernel = functools.partial(near_kernel, layout)
    near = call(kernel, 1, [piece] * pieces, place, hidden_in, gain, ids, limit=None)
    near = scatter(near)
    kernel = functools.partial(mark_kernel, layout)
    held = [pltpu.VMEM((slots, token_count), jnp.bfloat16), pltpu.VMEM(gain.shape, gain.dtype)]
    near_marks, far_marks, chosen, gain = call(kernel, 1, [marks, marks, *held], place, gain, ids, far_ids)
    far = scatter(call(far_kernel, 0, [piece] * pieces, far_hidden, gain, chosen))
    near = experts("near_experts", near)
    far = experts("far_experts", far)
    far = scatter(far)
    near = scatter(near)
    (partial,) = call(partial_kernel, 0, [array(token_count, model_width)], far_weights, far_marks, *far)
    partial = cross(partial)
    out = jax.ShapeDtypeStruct((token_count, model_width), jnp.bfloat16)
    return call(final_kernel, 0, [out], weights, near_marks, partial, *near)[0]


def solution(mesh):
    sizes = dict(mesh.shape)
    split = Mesh(mesh.devices.reshape(sizes["grp"], 2, sizes["ep"] // 2, sizes["tp"]), ("grp", "eh", "el", "tp"))
    rows, experts = P(("grp", "eh", "el", "tp"), None), P(("eh", "el", "tp"), None, None)

    def step(*args):
        return body(*args)

    step = jax.shard_map(
        step,
        mesh=split,
        in_specs=(rows, rows, rows, P(), experts, experts, experts),
        out_specs=rows,
        check_vma=False,
    )
    return step
```
